32 devices in a mesh: sp: 16 (over z, y, core), tp: 2 (over x).
Axes of the slice: x: 2, y: 2, z: 4, core: 2. Of those that a mesh axis runs over, the one named last changes fastest.
Arguments:
- tokens: bfloat16 [4096, 2048], P('sp', 'tp'), may hold values from -64 to 64
- input_norm_gain: float32 [2048], replicated, may hold values from 0.1 to 1.9
- attention_query_weight: bfloat16 [2048, 512], P(None, 'tp'), may hold values from -0.21875 to 0.21875
- attention_key_weight: bfloat16 [2048, 512], P(None, 'tp'), may hold values from -0.21875 to 0.21875
- attention_value_weight: bfloat16 [2048, 512], P(None, 'tp'), may hold values from -0.125 to 0.125
- attention_score_bias: float32 [8], P('tp'), may hold values from -18 to -7
- recurrence_query_weight: bfloat16 [2048, 1024], P(None, 'tp'), may hold values from -0.125 to 0.125
- forget_weight: bfloat16 [2048, 1024], P(None, 'tp'), may hold values from -0.125 to 0.125
- input_weight: bfloat16 [2048, 512], P(None, 'tp'), may hold values from -0.125 to 0.125
- output_gate_weight: bfloat16 [2048, 512], P(None, 'tp'), may hold values from -0.125 to 0.125
- forget_minimum: float32 [8, 128], P('tp'), may hold values from 0.9 to 1
- decay_spikes: float32 [4096, 8], P('sp', 'tp'), may hold values from -2.2 to 0
- head_norm_gain: float32 [64], replicated, may hold values from 0.1 to 1.9
- attention_output_weight: bfloat16 [512, 2048], P('tp'), may hold values from -0.25 to 0.25
- recurrence_output_weight: bfloat16 [512, 2048], P('tp'), may hold values from -0.25 to 0.25
Outputs:
- mixed: bfloat16 [4096, 2048], P('sp', 'tp')
The draws below stay inside these ranges and needn't reach their ends.
All inputs are finite; a program needn't handle non-finite values.
Results may differ from the reference program's by a relative error of at most 0.018.
Values may be sent and summed in bfloat16 or wider, within the bound.
No kernel may reach another device: no remote copies, remote signals or barrier semaphores. Data moves between devices by JAX's collectives and lax.ppermute only.
A program may use at most 64 MiB of HBM per device.

```python
import jax
import jax.numpy as jnp
from jax import lax

D = 2048
SB_HEADS = 8
HEAD = 64
REC_HEADS = 8
REC_KEY = 128
REC_VAL = 64
TOK_DEV = 256
REC_SPAN = 64
TOKENS = 4096


def draw_tokens(key, part):
    streams = jax.random.split(jax.random.fold_in(key, 11), 3)
    column_rise = jnp.exp(jnp.log(4.0) * jnp.arange(D, dtype=jnp.float32) / D)
    column_rough = jnp.exp(jax.random.uniform(streams[0], (D,), jnp.float32, -0.35, 0.35))
    row_scale = jnp.exp(jax.random.uniform(streams[1], (TOKENS, 1), jnp.float32, -0.7, 0.7))
    noise_field = jnp.clip(jax.random.normal(streams[2], (TOKENS, D), jnp.float32), -5.0, 5.0)
    return (noise_field * row_scale * column_rise[None, :] * column_rough[None, :]).astype(jnp.bfloat16)


def draw_attention_score_bias(key, part):
    spread = jax.random.uniform(jax.random.fold_in(key, 23), (SB_HEADS,), jnp.float32, jnp.log(0.3), jnp.log(3.0))
    return spread - jnp.log(90.0 * TOKENS)


def draw_forget_minimum(key, part):
    streams = jax.random.split(jax.random.fold_in(key, 31), 3)
    ranking = jax.random.permutation(streams[0], REC_HEADS)
    slow_count = REC_HEADS // 2
    is_slow = (ranking < slow_count)[:, None]
    slow_gap = jnp.exp(jax.random.uniform(streams[1], (REC_HEADS, REC_KEY), jnp.float32, jnp.log(0.2), jnp.log(1.2))) / TOKENS
    fast_gap = jnp.exp(jax.random.uniform(streams[2], (REC_HEADS, REC_KEY), jnp.float32, jnp.log(0.04), jnp.log(0.1)))
    return 1.0 - jnp.where(is_slow, slow_gap, fast_gap)


def draw_decay_spikes(key, part):
    streams = jax.random.split(jax.random.fold_in(key, 47), 3)
    block_count = TOKENS // TOK_DEV
    block_rate = jnp.exp(jax.random.uniform(streams[0], (block_count, 1, REC_HEADS), jnp.float32, jnp.log(0.15), jnp.log(0.6))) / TOKENS
    steady = -jnp.broadcast_to(block_rate, (block_count, TOK_DEV, REC_HEADS)).reshape(TOKENS, REC_HEADS)
    places = jax.random.randint(streams[1], (3, REC_HEADS), 0, TOKENS)
    struck = jnp.arange(TOKENS, dtype=jnp.int32)[:, None, None] == places[None]
    depth = jnp.log(jax.random.uniform(streams[2], (3, REC_HEADS), jnp.float32, 0.5, 0.8))
    return steady + jnp.sum(jnp.where(struck, depth[None], 0.0), axis=1)


def steps_of(rng, shape, cuts, low, top_value):
    def one(dim, blocks):
        heights = jax.random.uniform(jax.random.fold_in(jax.random.fold_in(rng, 6), dim), (blocks,), jnp.float32, low / len(cuts), top_value / len(cuts))
        return jnp.repeat(jnp.exp(heights), shape[dim] // blocks).reshape((-1,) + (1,) * (len(shape) - dim - 1))

    gain = one(*cuts[0])
    for cut in cuts[1:]:
        gain = gain * one(*cut)
    return gain


def normal_values(rng, extent, scale, reach, cuts=(), kind=jnp.bfloat16):
    entries = jax.random.normal(rng, extent, jnp.float32) * scale
    if len(cuts) > 0:
        entries = steps_of(rng, extent, cuts, -0.22, 0.18) * entries
    return jnp.clip(entries, min=-reach, max=reach).astype(kind)


def setup_inputs(seed: int = 0) -> dict:
    arg_keys = jax.random.split(jax.random.key(seed), 16)
    return {
        "tokens": draw_tokens(jax.random.fold_in(arg_keys[15], 71), 0),
        "input_norm_gain": jnp.clip(1.0 + 0.18 * jax.random.normal(arg_keys[1], (D,), jnp.float32), 0.1, 1.9),
        "attention_query_weight": normal_values(arg_keys[2], (D, SB_HEADS * HEAD), (D // 3) ** -0.5, 0.21875, ((1, 2),)),
        "attention_key_weight": normal_values(arg_keys[3], (D, SB_HEADS * HEAD), (D // 3) ** -0.5, 0.21875, ((1, 2),)),
        "attention_value_weight": normal_values(arg_keys[4], (D, SB_HEADS * HEAD), D ** -0.5, 0.125, ((1, 2),)),
        "attention_score_bias": draw_attention_score_bias(jax.random.fold_in(arg_keys[15], 71), 0),
        "recurrence_query_weight": normal_values(arg_keys[6], (D, REC_HEADS * REC_KEY), D ** -0.5, 0.125, ((1, 2),)),
        "forget_weight": normal_values(arg_keys[7], (D, REC_HEADS * REC_KEY), D ** -0.5, 0.125, ((1, 2),)),
        "input_weight": normal_values(arg_keys[8], (D, REC_HEADS * REC_VAL), D ** -0.5, 0.125, ((1, 2),)),
        "output_gate_weight": normal_values(arg_keys[9], (D, REC_HEADS * REC_VAL), D ** -0.5, 0.125, ((1, 2),)),
        "forget_minimum": draw_forget_minimum(jax.random.fold_in(arg_keys[15], 71), 0),
        "decay_spikes": draw_decay_spikes(jax.random.fold_in(arg_keys[15], 71), 0),
        "head_norm_gain": jnp.clip(1.0 + 0.18 * jax.random.normal(arg_keys[12], (REC_VAL,), jnp.float32), 0.1, 1.9),
        "attention_output_weight": normal_values(arg_keys[13], (SB_HEADS * HEAD, D), (SB_HEADS * HEAD) ** -0.5, 0.25, ((0, 2),)),
        "recurrence_output_weight": normal_values(arg_keys[14], (REC_HEADS * REC_VAL, D), (REC_HEADS * REC_VAL) ** -0.5, 0.25, ((0, 2),)),
    }


epsilon = 1e-06

def project(scaled, inverse, weight):
    return (jnp.dot(scaled, weight, preferred_element_type=jnp.float32) * inverse).astype(jnp.bfloat16)

def stick_breaking(query_stick, key_stick, value_stick, attention_score_bias):
    block_count = TOKENS // TOK_DEV
    query_blocks = query_stick.reshape(block_count, TOK_DEV, SB_HEADS, HEAD)
    key_heads = key_stick.reshape(TOKENS, SB_HEADS, HEAD).astype(jnp.float32)
    value_heads = value_stick.reshape(TOKENS, SB_HEADS, HEAD).astype(jnp.float32)
    key_pos = jnp.arange(TOKENS, dtype=jnp.int32)

    def one_block(inputs):
        query_block, number = inputs
        query_pos = number * TOK_DEV + jnp.arange(TOK_DEV, dtype=jnp.int32)
        scores = jnp.einsum('qhd,khd->hqk', query_block.astype(jnp.float32), key_heads) * HEAD ** (-0.5)
        scores = scores + attention_score_bias[:, None, None]
        before = (key_pos[None, :] < query_pos[:, None])[None]
        log_rest = jnp.where(before, jax.nn.log_sigmoid(-scores), 0.0)
        later_sum = lax.cumsum(log_rest, axis=2, reverse=True) - log_rest
        weights = jnp.where(before, jnp.exp(jax.nn.log_sigmoid(scores) + later_sum), 0.0).astype(jnp.bfloat16)
        final_output = jnp.einsum('hqk,khd->qhd', weights.astype(jnp.float32), value_heads)
        return final_output.reshape(TOK_DEV, SB_HEADS * HEAD).astype(jnp.bfloat16)
    blocks = lax.map(one_block, (query_blocks, jnp.arange(block_count, dtype=jnp.int32)))
    return blocks.reshape(TOKENS, SB_HEADS * HEAD)

def linear_recurrence(query_rows, forget_rows, input_rows, gate_rows, forget_minimum, decay_spikes, head_norm_gain):
    peak_value = lax.Precision.HIGHEST
    raised_values = jax.nn.silu(query_rows.astype(jnp.float32)).reshape(TOKENS, REC_HEADS, REC_KEY)
    admitted_input = (1.0 - forget_minimum)[None] * jax.nn.sigmoid(-forget_rows.astype(jnp.float32).reshape(TOKENS, REC_HEADS, REC_KEY))
    forget_logarithm = jnp.log1p(-admitted_input) + decay_spikes[:, :, None]
    inputs = input_rows.astype(jnp.float32).reshape(TOKENS, REC_HEADS, REC_VAL)
    span_count = TOKENS // REC_SPAN
    causal = jnp.tril(jnp.ones((REC_SPAN, REC_SPAN), jnp.bool_))[:, :, None, None]

    def to_spans(array):
        return array.reshape(span_count, REC_SPAN, REC_HEADS, array.shape[-1])

    def advance(recurrent_memory, pieces):
        window_query, window_admitted, window_input, span_log = pieces
        running_total = jnp.cumsum(span_log, axis=0)
        log_gaps = running_total[:, None] - running_total[None, :]
        decay_table = jnp.where(causal, jnp.exp(jnp.where(causal, log_gaps, 0.0)), 0.0)
        inner_scores = jnp.einsum('thk,shk,tshk->hts', window_query, window_admitted, decay_table, precision=peak_value)
        final_output = jnp.einsum('hts,shv->thv', inner_scores, window_input, precision=peak_value)
        final_output = final_output + jnp.einsum('zbg,bgp->zbp', window_query * jnp.exp(running_total), recurrent_memory, precision=peak_value)
        window_total = running_total[-1]
        recurrent_memory = recurrent_memory * jnp.exp(window_total)[:, :, None] + jnp.einsum('rof,roi->ofi', window_admitted * jnp.exp(window_total[None] - running_total), window_input, precision=peak_value)
        return (recurrent_memory, final_output)
    start_memory = jnp.zeros((REC_HEADS, REC_KEY, REC_VAL), jnp.float32)
    memory_end, outputs = lax.scan(advance, start_memory, (to_spans(raised_values), to_spans(admitted_input), to_spans(inputs), to_spans(forget_logarithm)))
    outputs = outputs.reshape(TOKENS, REC_HEADS, REC_VAL)
    normed = outputs * lax.rsqrt(lax.optimization_barrier(jnp.mean(outputs * outputs, axis=2, keepdims=True)) + epsilon) * head_norm_gain
    gated_out = normed * jax.nn.silu(gate_rows.astype(jnp.float32).reshape(TOKENS, REC_HEADS, REC_VAL))
    return gated_out.reshape(TOKENS, REC_HEADS * REC_VAL).astype(jnp.bfloat16)

def reference(tokens, input_norm_gain, attention_query_weight, attention_key_weight, attention_value_weight, attention_score_bias, recurrence_query_weight, forget_weight, input_weight, output_gate_weight, forget_minimum, decay_spikes, head_norm_gain, attention_output_weight, recurrence_output_weight):
    values = tokens.astype(jnp.float32)
    scaled = (values * input_norm_gain[None, :]).astype(jnp.bfloat16)
    inverse = lax.rsqrt(lax.optimization_barrier(jnp.mean(values * values, axis=1, keepdims=True)) + epsilon)
    query_stick = project(scaled, inverse, attention_query_weight)
    key_stick = project(scaled, inverse, attention_key_weight)
    value_stick = project(scaled, inverse, attention_value_weight)
    query_rows = project(scaled, inverse, recurrence_query_weight)
    forget_rows = project(scaled, inverse, forget_weight)
    input_rows = project(scaled, inverse, input_weight)
    gate_rows = project(scaled, inverse, output_gate_weight)
    stick_heads = stick_breaking(query_stick, key_stick, value_stick, attention_score_bias)
    recurrence_heads = linear_recurrence(query_rows, forget_rows, input_rows, gate_rows, forget_minimum, decay_spikes, head_norm_gain)
    mixed_out = jnp.dot(stick_heads, attention_output_weight, preferred_element_type=jnp.float32)
    mixed_out = mixed_out + jnp.dot(recurrence_heads, recurrence_output_weight, preferred_element_type=jnp.float32)
    return mixed_out.astype(jnp.bfloat16)
```

```python
import jax
import jax.numpy as jnp
from jax import lax
from jax.experimental import pallas as pl
from jax.experimental.pallas import tpu as pltpu
from jax.sharding import PartitionSpec as P

HEAD = 64
REC_KEY = 128
REC_VAL = 64
LANES = 128
STATE_ROWS = 72
epsilon = 1e-06
F32 = jnp.float32
BF16 = jnp.bfloat16
EXACT = lax.Precision.HIGHEST


def dot(a, b, dims=((1,), (0,)), precision=None):
    return lax.dot_general(a, b, (dims, ((), ())), precision=precision, preferred_element_type=F32)


def tri(n, compare):
    row = lax.broadcasted_iota(jnp.int32, (n, n), 0)
    col = lax.broadcasted_iota(jnp.int32, (n, n), 1)
    return compare(row, col)


def project(tokens, gain, weights):
    rows, width = tokens.shape
    step = 256
    steps = width // step
    cols = [w.shape[1] for w in weights]

    def body(x_ref, g_ref, *refs):
        w_refs = refs[:7]
        q_ref, kv_ref, rq_ref, rf_ref, ri_ref, rg_ref = refs[7:13]
        accs = refs[13:20]
        sq_ref = refs[20]
        i = pl.program_id(0)
        x = x_ref[...].astype(F32)
        scaled = (x * g_ref[...]).astype(BF16)
        squares = jnp.sum(x * x, axis=1, keepdims=True)

        @pl.when(i == 0)
        def _():
            sq_ref[...] = squares
            for acc, w in zip(accs, w_refs):
                acc[...] = dot(scaled, w[...])

        @pl.when(i > 0)
        def _():
            sq_ref[...] += squares
            for acc, w in zip(accs, w_refs):
                acc[...] += dot(scaled, w[...])

        @pl.when(i == steps - 1)
        def _():
            inverse = lax.rsqrt(sq_ref[...] / width + epsilon)
            done = [(acc[...] * inverse).astype(BF16) for acc in accs]
            q_ref[...] = done[0]
            kv_ref[:, : cols[1]] = done[1]
            kv_ref[:, cols[1] :] = done[2]
            rq_ref[...] = done[3]
            rf_ref[...] = done[4]
            ri_ref[...] = done[5]
            rg_ref[...] = done[6]

    outs = [cols[0], cols[1] + cols[2], *cols[3:]]
    return pl.pallas_call(
        body,
        grid=(steps,),
        in_specs=[
            pl.BlockSpec((rows, step), lambda i: (0, i)),
            pl.BlockSpec((1, step), lambda i: (0, i)),
            *[pl.BlockSpec((step, c), lambda i: (i, 0)) for c in cols],
        ],
        out_specs=[pl.BlockSpec((rows, c), lambda i: (0, 0)) for c in outs],
        out_shape=[jax.ShapeDtypeStruct((rows, c), BF16) for c in outs],
        scratch_shapes=[pltpu.VMEM((rows, c), F32) for c in cols] + [pltpu.VMEM((rows, 1), F32)],
        name="project",
    )(tokens, gain[None, :], *weights)


def stick(place, bias, query, keys_values):
    rows, width = query.shape
    total = keys_values.shape[0]
    slab = min(LANES, width)
    slabs = width // slab
    per = slab // HEAD
    if slab % LANES == 0:
        keys, values, shift = keys_values, keys_values, slabs
    else:
        keys, values, shift = keys_values[:, :width], keys_values[:, width:], 0

    def body(place_ref, bias_ref, q_ref, k_ref, v_ref, o_ref, acc_ref, carry_ref, tri_ref):
        p = pl.program_id(0)
        here = place_ref[0]
        lane = lax.broadcasted_iota(jnp.int32, (rows, slab), 1) // HEAD
        scaled = q_ref[...] * jnp.asarray(HEAD**-0.5, BF16)
        heads = [jnp.where(lane == h, scaled, jnp.zeros_like(scaled)) for h in range(per)]
        tri_ref[...] = jnp.where(tri(rows, lambda r, c: r > c), 1.0, 0.0).astype(BF16)

        def block(number, diagonal):
            start = pl.multiple_of(number * rows, rows)
            key = k_ref[pl.ds(start, rows), :]
            value = v_ref[pl.ds(start, rows), :]
            for h in range(per):
                score = dot(heads[h], key, ((1,), (1,))) + bias_ref[p * per + h]
                small = jnp.log(1.0 + jnp.exp(-jnp.abs(score)))
                rest = jnp.maximum(score, 0.0) + small
                take = jnp.minimum(score, 0.0) - small
                if diagonal:
                    before = tri(rows, lambda r, c: c < r)
                    rest = jnp.where(before, rest, 0.0)
                later = dot(rest.astype(BF16), tri_ref[...])
                gone = later[:, 0:1] + rest[:, 0:1]
                if diagonal:
                    weight = jnp.where(before, jnp.exp(take - later), 0.0)
                else:
                    weight = jnp.exp(take - later - carry_ref[h])
                part = jnp.where(lane == h, dot(weight.astype(BF16), value), 0.0)
                if diagonal and h == 0:
                    acc_ref[...] = part
                else:
                    acc_ref[...] += part
                if diagonal:
                    carry_ref[h] = gone
                else:
                    carry_ref[h] += gone

        block(here, True)

        @pl.loop(0, here)
        def _(i):
            block(here - 1 - i, False)

        o_ref[...] = acc_ref[...].astype(BF16)

    return pl.pallas_call(
        body,
        grid=(slabs,),
        in_specs=[
            pl.BlockSpec(memory_space=pltpu.SMEM),
            pl.BlockSpec(memory_space=pltpu.SMEM),
            pl.BlockSpec((rows, slab), lambda p: (0, p)),
            pl.BlockSpec((total, slab), lambda p: (0, p)),
            pl.BlockSpec((total, slab), lambda p: (0, shift + p)),
        ],
        out_specs=pl.BlockSpec((rows, slab), lambda p: (0, p)),
        out_shape=jax.ShapeDtypeStruct((rows, width), BF16),
        scratch_shapes=[
            pltpu.VMEM((rows, slab), F32),
            pltpu.VMEM((per, rows, 1), F32),
            pltpu.VMEM((rows, rows), BF16),
        ],
        name="stick",
    )(place, bias, query, keys, values)


def local_recurrence(query, forget, inputs, minimum, spikes):
    rows = query.shape[0]
    heads = minimum.shape[0]
    width = heads * REC_VAL
    slab = min(LANES, width)
    per = slab // REC_VAL

    def body(q_ref, f_ref, x_ref, m_ref, s_ref, st_ref, raw_ref, qd_ref, state_ref):
        causal = tri(rows, lambda r, c: c <= r)
        lower = jnp.where(causal, 1.0, 0.0)
        spike_col = dot(lower, s_ref[...], precision=EXACT)
        spike_row = dot(st_ref[...], lower, ((1,), (1,)), precision=EXACT)
        lane = lax.broadcasted_iota(jnp.int32, (rows, slab), 1) // REC_VAL
        for p in range(width // slab):
            x = x_ref[:, p * slab : (p + 1) * slab]
            raw = None
            for hh in range(per):
                h = p * per + hh
                keys = slice(h * REC_KEY, (h + 1) * REC_KEY)
                q = q_ref[:, keys].astype(F32)
                lifted = q * jax.nn.sigmoid(q)
                intake = (1.0 - m_ref[h : h + 1, :]) * jax.nn.sigmoid(-f_ref[:, keys].astype(F32))
                gap = dot(lower, jnp.log1p(-intake), precision=EXACT)
                middle = gap[rows // 2 : rows // 2 + 1, :]
                column = spike_col[:, h : h + 1]
                across = spike_row[h : h + 1, :]
                up = (lifted * jnp.exp(gap - middle)).astype(BF16)
                down = (intake * jnp.exp(middle - gap)).astype(BF16)
                table = jnp.where(causal, jnp.exp(jnp.minimum(column - across, 0.0)), 0.0)
                inner = dot(up, down, ((1,), (1,)))
                inner = (jnp.where(causal, inner, 0.0) * table).astype(BF16)
                own = jnp.where(lane == hh, x, jnp.zeros_like(x))
                part = dot(inner, own)
                raw = part if raw is None else raw + part
                whole = gap + column
                last = whole[rows - 1 : rows, :]
                qd_ref[:, keys] = (lifted * jnp.exp(whole)).astype(BF16)
                leaving = (intake * jnp.exp(last - whole)).astype(BF16)
                memory = dot(x, leaving, ((0,), (0,)))
                state_ref[h, :REC_VAL, :] = memory[hh * REC_VAL : (hh + 1) * REC_VAL, :]
                state_ref[h, REC_VAL:, :] = jnp.broadcast_to(
                    jnp.exp(last), (STATE_ROWS - REC_VAL, REC_KEY)
                )
            raw_ref[:, p * slab : (p + 1) * slab] = raw

    return pl.pallas_call(
        body,
        out_shape=[
            jax.ShapeDtypeStruct((rows, width), F32),
            jax.ShapeDtypeStruct((rows, heads * REC_KEY), BF16),
            jax.ShapeDtypeStruct((heads, STATE_ROWS, REC_KEY), F32),
        ],
        name="local_recurrence",
    )(query, forget, inputs, minimum, spikes, spikes.T)


def finish_recurrence(place, raw, decayed, states, gate, gain):
    rows, width = raw.shape
    heads = width // REC_VAL
    slab = min(LANES, width)
    per = slab // REC_VAL

    def body(place_ref, raw_ref, qd_ref, st_ref, g_ref, n_ref, o_ref, s_ref):
        s_ref[...] = jnp.zeros_like(s_ref)

        @pl.loop(0, place_ref[0])
        def _(j):
            for h in range(heads):
                s_ref[h] = s_ref[h] * st_ref[j, h, REC_VAL : REC_VAL + 1, :] + st_ref[j, h, :REC_VAL, :]

        lane = lax.broadcasted_iota(jnp.int32, (rows, slab), 1) // REC_VAL
        for p in range(width // slab):
            cut = slice(p * slab, (p + 1) * slab)
            out = raw_ref[:, cut]
            for hh in range(per):
                h = p * per + hh
                state = s_ref[h].astype(BF16)
                blank = jnp.zeros_like(state)
                if per > 1:
                    state = jnp.concatenate([state if k == hh else blank for k in range(per)], axis=0)
                out = out + dot(qd_ref[:, h * REC_KEY : (h + 1) * REC_KEY], state, ((1,), (1,)))
            square = out * out
            scale = jnp.zeros_like(out)
            for hh in range(per):
                mean = jnp.sum(jnp.where(lane == hh, square, 0.0), axis=1, keepdims=True) / REC_VAL
                scale = jnp.where(lane == hh, lax.rsqrt(mean + epsilon), scale)
            gated = g_ref[:, cut].astype(F32)
            out = out * scale * n_ref[...] * (gated * jax.nn.sigmoid(gated))
            o_ref[:, cut] = out.astype(BF16)

    vmem = pl.BlockSpec(memory_space=pltpu.VMEM)
    return pl.pallas_call(
        body,
        in_specs=[pl.BlockSpec(memory_space=pltpu.SMEM), vmem, vmem, vmem, vmem, vmem],
        out_specs=vmem,
        out_shape=jax.ShapeDtypeStruct((rows, width), BF16),
        scratch_shapes=[pltpu.VMEM((heads, REC_VAL, REC_KEY), F32)],
        name="finish_recurrence",
    )(place, raw, decayed, states, gate, jnp.tile(gain, per)[None, :])


def shards(
    tokens,
    input_norm_gain,
    attention_query_weight,
    attention_key_weight,
    attention_value_weight,
    attention_score_bias,
    recurrence_query_weight,
    forget_weight,
    input_weight,
    output_gate_weight,
    forget_minimum,
    decay_spikes,
    head_norm_gain,
    attention_output_weight,
    recurrence_output_weight,
):
    parts = lax.axis_size("tp")
    mine = lax.axis_index("tp")
    place = lax.axis_index("sp").astype(jnp.int32)[None]
    pair = parts == 2
    swap = [(0, 1), (1, 0)]
    features = tokens.shape[1]
    if pair:
        other = lax.ppermute(tokens, "tp", swap)
        full = jnp.where(
            mine == 0,
            jnp.concatenate([tokens, other], axis=1),
            jnp.concatenate([other, tokens], axis=1),
        )
        att_w, rec_w, full = lax.optimization_barrier(
            (attention_output_weight, recurrence_output_weight, full)
        )

        def half(array, which):
            return lax.dynamic_slice_in_dim(array, which * features, features, 1)

        sent_att = lax.ppermute(half(att_w, 1 - mine), "tp", swap)
        sent_rec = lax.ppermute(half(rec_w, 1 - mine), "tp", swap)
    else:
        full = lax.all_gather(tokens, "tp", axis=1, tiled=True)
    query, keys_values, rec_query, rec_forget, rec_input, rec_gate = project(
        full,
        input_norm_gain,
        (
            attention_query_weight,
            attention_key_weight,
            attention_value_weight,
            recurrence_query_weight,
            forget_weight,
            input_weight,
            output_gate_weight,
        ),
    )
    all_pairs = lax.all_gather(keys_values, "sp", axis=0, tiled=True)
    raw, decayed, state = local_recurrence(
        rec_query, rec_forget, rec_input, forget_minimum, decay_spikes
    )
    states = lax.all_gather(state, "sp")
    state_heads = finish_recurrence(place, raw, decayed, states, rec_gate, head_norm_gain)
    if pair:
        other_state = lax.ppermute(state_heads, "tp", swap)
    stick_heads = stick(place, attention_score_bias, query, all_pairs)
    if pair:
        other_stick = lax.ppermute(stick_heads, "tp", swap)
        mixed = dot(state_heads, half(rec_w, mine)) + dot(other_state, sent_rec)
        mixed = mixed + dot(stick_heads, half(att_w, mine)) + dot(other_stick, sent_att)
    else:
        stick_all = lax.all_gather(stick_heads, "tp", axis=1, tiled=True)
        state_all = lax.all_gather(state_heads, "tp", axis=1, tiled=True)
        att_cols = lax.all_to_all(
            attention_output_weight, "tp", split_axis=1, concat_axis=0, tiled=True
        )
        rec_cols = lax.all_to_all(
            recurrence_output_weight, "tp", split_axis=1, concat_axis=0, tiled=True
        )
        mixed = dot(stick_all, att_cols) + dot(state_all, rec_cols)
    return mixed.astype(BF16)


def solution(mesh):
    placed = (
        P("sp", "tp"),
        P(),
        P(None, "tp"),
        P(None, "tp"),
        P(None, "tp"),
        P("tp"),
        P(None, "tp"),
        P(None, "tp"),
        P(None, "tp"),
        P(None, "tp"),
        P("tp", None),
        P("sp", "tp"),
        P(),
        P("tp", None),
        P("tp", None),
    )
    return jax.shard_map(
        shards, mesh=mesh, in_specs=placed, out_specs=P("sp", "tp"), check_vma=False
    )
```

```python
import jax
import jax.numpy as jnp
from jax import lax
from jax.experimental import pallas as pl
from jax.experimental.pallas import tpu as pltpu
from jax.sharding import PartitionSpec as P

HEAD = 64
REC_KEY = 128
REC_VAL = 64
LANES = 128
STATE_ROWS = 72
epsilon = 1e-06
F32 = jnp.float32
BF16 = jnp.bfloat16
EXACT = lax.Precision.HIGHEST


def dot(a, b, dims=((1,), (0,)), precision=None):
    return lax.dot_general(a, b, (dims, ((), ())), precision=precision, preferred_element_type=F32)


def tri(n, compare):
    row = lax.broadcasted_iota(jnp.int32, (n, n), 0)
    col = lax.broadcasted_iota(jnp.int32, (n, n), 1)
    return compare(row, col)


def project(tokens, gain, weights):
    rows, width = tokens.shape
    step = 256
    steps = width // step
    cols = [w.shape[1] for w in weights]

    def body(x_ref, g_ref, *refs):
        w_refs = refs[:7]
        q_ref, kv_ref, rq_ref, rf_ref, ri_ref, rg_ref = refs[7:13]
        accs = refs[13:20]
        sq_ref = refs[20]
        i = pl.program_id(0)
        x = x_ref[...].astype(F32)
        scaled = (x * g_ref[...]).astype(BF16)
        squares = jnp.sum(x * x, axis=1, keepdims=True)

        @pl.when(i == 0)
        def _():
            sq_ref[...] = squares
            for acc, w in zip(accs, w_refs):
                acc[...] = dot(scaled, w[...])

        @pl.when(i > 0)
        def _():
            sq_ref[...] += squares
            for acc, w in zip(accs, w_refs):
                acc[...] += dot(scaled, w[...])

        @pl.when(i == steps - 1)
        def _():
            inverse = lax.rsqrt(sq_ref[...] / width + epsilon)
            done = [(acc[...] * inverse).astype(BF16) for acc in accs]
            q_ref[...] = done[0]
            kv_ref[:, : cols[1]] = done[1]
            kv_ref[:, cols[1] :] = done[2]
            rq_ref[...] = done[3]
            rf_ref[...] = done[4]
            ri_ref[...] = done[5]
            rg_ref[...] = done[6]

    outs = [cols[0], cols[1] + cols[2], *cols[3:]]
    return pl.pallas_call(
        body,
        grid=(steps,),
        in_specs=[
            pl.BlockSpec((rows, step), lambda i: (0, i)),
            pl.BlockSpec((1, step), lambda i: (0, i)),
            *[pl.BlockSpec((step, c), lambda i: (i, 0)) for c in cols],
        ],
        out_specs=[pl.BlockSpec((rows, c), lambda i: (0, 0)) for c in outs],
        out_shape=[jax.ShapeDtypeStruct((rows, c), BF16) for c in outs],
        scratch_shapes=[pltpu.VMEM((rows, c), F32) for c in cols] + [pltpu.VMEM((rows, 1), F32)],
        name="project",
    )(tokens, gain[None, :], *weights)


def stick(place, bias, query, pieces, plane):
    rows, width = query.shape
    count = sum(piece.shape[0] for piece in pieces) // rows
    slab = min(LANES, width)
    per = slab // HEAD

    def body(place_ref, bias_ref, q_ref, *refs):
        piece_refs = refs[: len(pieces)]
        o_ref, kv_ref, acc_ref, carry_ref, tri_ref, sems = refs[len(pieces) :]
        copies = []
        offset = 0
        for k, piece in enumerate(piece_refs):
            size = piece.shape[0]
            copies.append(
                pltpu.make_async_copy(piece, kv_ref.at[pl.ds(offset, size), :], sems.at[k])
            )
            offset += size
        for copy in copies:
            copy.start()
        here = place_ref[0]
        lane = lax.broadcasted_iota(jnp.int32, (rows, slab), 1) // HEAD
        tri_ref[...] = jnp.where(tri(rows, lambda r, c: r > c), 1.0, 0.0).astype(BF16)
        for copy in copies:
            copy.wait()

        def slot_of(number):
            if plane == 1:
                return number
            away = here // plane - number // plane
            return away * plane + ((number % plane) ^ (here % plane))

        for p in range(width // slab):
            scaled = q_ref[:, p * slab : (p + 1) * slab] * jnp.asarray(HEAD**-0.5, BF16)
            heads = [jnp.where(lane == h, scaled, jnp.zeros_like(scaled)) for h in range(per)]

            def block(number, diagonal):
                start = pl.multiple_of(slot_of(number) * rows, rows)
                key = kv_ref[pl.ds(start, rows), p * slab : (p + 1) * slab]
                value = kv_ref[pl.ds(start, rows), width + p * slab : width + (p + 1) * slab]
                for h in range(per):
                    score = dot(heads[h], key, ((1,), (1,))) + bias_ref[p * per + h]
                    small = jnp.log(1.0 + jnp.exp(-jnp.abs(score)))
                    rest = jnp.maximum(score, 0.0) + small
                    take = jnp.minimum(score, 0.0) - small
                    if diagonal:
                        before = tri(rows, lambda r, c: c < r)
                        rest = jnp.where(before, rest, 0.0)
                    later = dot(rest.astype(BF16), tri_ref[...])
                    gone = later[:, 0:1] + rest[:, 0:1]
                    if diagonal:
                        weight = jnp.where(before, jnp.exp(take - later), 0.0)
                    else:
                        weight = jnp.exp(take - later - carry_ref[h])
                    part = jnp.where(lane == h, dot(weight.astype(BF16), value), 0.0)
                    if diagonal and h == 0:
                        acc_ref[...] = part
                    else:
                        acc_ref[...] += part
                    if diagonal:
                        carry_ref[h] = gone
                    else:
                        carry_ref[h] += gone

            block(here, True)

            @pl.loop(0, here)
            def _(i):
                block(here - 1 - i, False)

            o_ref[:, p * slab : (p + 1) * slab] = acc_ref[...].astype(BF16)

    smem = pl.BlockSpec(memory_space=pltpu.SMEM)
    vmem = pl.BlockSpec(memory_space=pltpu.VMEM)
    return pl.pallas_call(
        body,
        in_specs=[smem, smem, vmem, *[pl.BlockSpec(memory_space=pl.ANY) for _ in pieces]],
        out_specs=vmem,
        out_shape=jax.ShapeDtypeStruct((rows, width), BF16),
        scratch_shapes=[
            pltpu.VMEM((count * rows, 2 * width), BF16),
            pltpu.VMEM((rows, slab), F32),
            pltpu.VMEM((per, rows, 1), F32),
            pltpu.VMEM((rows, rows), BF16),
            pltpu.SemaphoreType.DMA((len(pieces),)),
        ],
        name="stick",
    )(place, bias, query, *pieces)


def shifted(array, by):
    size = lax.axis_size("sp")
    return lax.ppermute(array, "sp", [(i, i + by) for i in range(size - by)])


def crossed(array, mask):
    size = lax.axis_size("sp")
    return lax.ppermute(array, "sp", [(i, i ^ mask) for i in range(size)])


def gathered(array):
    size = lax.axis_size("sp")
    if size % 4 or size > 16:
        return [lax.all_gather(array, "sp", axis=0, tiled=True)], 1
    firsts = [array] + [shifted(array, 4 * away) for away in range(1, size // 4)]
    pieces = []
    for first in firsts:
        across = crossed(first, 2)
        pieces += [first, crossed(first, 1), across, crossed(across, 1)]
    return pieces, 4


def entering(state):
    size = lax.axis_size("sp")
    row = lax.broadcasted_iota(jnp.int32, state.shape, 1)
    state = shifted(state, 1)
    by = 1
    while by < size:
        decay = state[:, REC_VAL : REC_VAL + 1, :]
        state = shifted(state, by) * decay + jnp.where(row < REC_VAL, state, 0.0)
        by *= 2
    return state


def local_recurrence(query, forget, inputs, minimum, spikes):
    rows = query.shape[0]
    heads = minimum.shape[0]
    width = heads * REC_VAL
    slab = min(LANES, width)
    per = slab // REC_VAL

    def body(q_ref, f_ref, x_ref, m_ref, s_ref, st_ref, raw_ref, qd_ref, state_ref):
        causal = tri(rows, lambda r, c: c <= r)
        lower = jnp.where(causal, 1.0, 0.0)
        spike_col = dot(lower, s_ref[...], precision=EXACT)
        spike_row = dot(st_ref[...], lower, ((1,), (1,)), precision=EXACT)
        lane = lax.broadcasted_iota(jnp.int32, (rows, slab), 1) // REC_VAL
        for p in range(width // slab):
            x = x_ref[:, p * slab : (p + 1) * slab]
            raw = None
            for hh in range(per):
                h = p * per + hh
                keys = slice(h * REC_KEY, (h + 1) * REC_KEY)
                q = q_ref[:, keys].astype(F32)
                lifted = q * jax.nn.sigmoid(q)
                intake = (1.0 - m_ref[h : h + 1, :]) * jax.nn.sigmoid(-f_ref[:, keys].astype(F32))
                gap = dot(lower, jnp.log1p(-intake), precision=EXACT)
                middle = gap[rows // 2 : rows // 2 + 1, :]
                column = spike_col[:, h : h + 1]
                across = spike_row[h : h + 1, :]
                up = (lifted * jnp.exp(gap - middle)).astype(BF16)
                down = (intake * jnp.exp(middle - gap)).astype(BF16)
                table = jnp.where(causal, jnp.exp(jnp.minimum(column - across, 0.0)), 0.0)
                inner = dot(up, down, ((1,), (1,)))
                inner = (jnp.where(causal, inner, 0.0) * table).astype(BF16)
                own = jnp.where(lane == hh, x, jnp.zeros_like(x))
                part = dot(inner, own)
                raw = part if raw is None else raw + part
                whole = gap + column
                last = whole[rows - 1 : rows, :]
                qd_ref[:, keys] = (lifted * jnp.exp(whole)).astype(BF16)
                leaving = (intake * jnp.exp(last - whole)).astype(BF16)
                memory = dot(x, leaving, ((0,), (0,)))
                state_ref[h, :REC_VAL, :] = memory[hh * REC_VAL : (hh + 1) * REC_VAL, :]
                state_ref[h, REC_VAL:, :] = jnp.broadcast_to(
                    jnp.exp(last), (STATE_ROWS - REC_VAL, REC_KEY)
                )
            raw_ref[:, p * slab : (p + 1) * slab] = raw

    return pl.pallas_call(
        body,
        out_shape=[
            jax.ShapeDtypeStruct((rows, width), F32),
            jax.ShapeDtypeStruct((rows, heads * REC_KEY), BF16),
            jax.ShapeDtypeStruct((heads, STATE_ROWS, REC_KEY), F32),
        ],
        name="local_recurrence",
    )(query, forget, inputs, minimum, spikes, spikes.T)


def finish_recurrence(raw, decayed, entered, gate, gain):
    rows, width = raw.shape
    slab = min(LANES, width)
    per = slab // REC_VAL

    def body(raw_ref, qd_ref, s_ref, g_ref, n_ref, o_ref):
        lane = lax.broadcasted_iota(jnp.int32, (rows, slab), 1) // REC_VAL
        for p in range(width // slab):
            cut = slice(p * slab, (p + 1) * slab)
            out = raw_ref[:, cut]
            for hh in range(per):
                h = p * per + hh
                state = s_ref[h, :REC_VAL, :].astype(BF16)
                blank = jnp.zeros_like(state)
                if per > 1:
                    state = jnp.concatenate([state if k == hh else blank for k in range(per)], axis=0)
                out = out + dot(qd_ref[:, h * REC_KEY : (h + 1) * REC_KEY], state, ((1,), (1,)))
            square = out * out
            scale = jnp.zeros_like(out)
            for hh in range(per):
                mean = jnp.sum(jnp.where(lane == hh, square, 0.0), axis=1, keepdims=True) / REC_VAL
                scale = jnp.where(lane == hh, lax.rsqrt(mean + epsilon), scale)
            gated = g_ref[:, cut].astype(F32)
            out = out * scale * n_ref[...] * (gated * jax.nn.sigmoid(gated))
            o_ref[:, cut] = out.astype(BF16)

    vmem = pl.BlockSpec(memory_space=pltpu.VMEM)
    return pl.pallas_call(
        body,
        in_specs=[vmem] * 5,
        out_specs=vmem,
        out_shape=jax.ShapeDtypeStruct((rows, width), BF16),
        name="finish_recurrence",
    )(raw, decayed, entered, gate, jnp.tile(gain, per)[None, :])


def shards(
    tokens,
    input_norm_gain,
    attention_query_weight,
    attention_key_weight,
    attention_value_weight,
    attention_score_bias,
    recurrence_query_weight,
    forget_weight,
    input_weight,
    output_gate_weight,
    forget_minimum,
    decay_spikes,
    head_norm_gain,
    attention_output_weight,
    recurrence_output_weight,
):
    parts = lax.axis_size("tp")
    mine = lax.axis_index("tp")
    place = lax.axis_index("sp").astype(jnp.int32)[None]
    pair = parts == 2
    swap = [(0, 1), (1, 0)]
    features = tokens.shape[1]
    if pair:
        other = lax.ppermute(tokens, "tp", swap)
        full = jnp.where(
            mine == 0,
            jnp.concatenate([tokens, other], axis=1),
            jnp.concatenate([other, tokens], axis=1),
        )
        att_w, rec_w, full = lax.optimization_barrier(
            (attention_output_weight, recurrence_output_weight, full)
        )

        def half(array, which):
            return lax.dynamic_slice_in_dim(array, which * features, features, 1)

        sent_att = lax.ppermute(half(att_w, 1 - mine), "tp", swap)
        sent_rec = lax.ppermute(half(rec_w, 1 - mine), "tp", swap)
    else:
        full = lax.all_gather(tokens, "tp", axis=1, tiled=True)
    query, keys_values, rec_query, rec_forget, rec_input, rec_gate = project(
        full,
        input_norm_gain,
        (
            attention_query_weight,
            attention_key_weight,
            attention_value_weight,
            recurrence_query_weight,
            forget_weight,
            input_weight,
            output_gate_weight,
        ),
    )
    pieces, plane = gathered(keys_values)
    raw, decayed, state = local_recurrence(
        rec_query, rec_forget, rec_input, forget_minimum, decay_spikes
    )
    if plane > 1:
        state, *pieces[::plane] = lax.optimization_barrier((state, *pieces[::plane]))
    state_heads = finish_recurrence(raw, decayed, entering(state), rec_gate, head_norm_gain)
    if pair:
        other_state = lax.ppermute(state_heads, "tp", swap)
    stick_heads = stick(place, attention_score_bias, query, pieces, plane)
    if pair:
        other_stick = lax.ppermute(stick_heads, "tp", swap)
        mixed = dot(state_heads, half(rec_w, mine)) + dot(other_state, sent_rec)
        mixed = mixed + dot(stick_heads, half(att_w, mine)) + dot(other_stick, sent_att)
    else:
        stick_all = lax.all_gather(stick_heads, "tp", axis=1, tiled=True)
        state_all = lax.all_gather(state_heads, "tp", axis=1, tiled=True)
        att_cols = lax.all_to_all(
            attention_output_weight, "tp", split_axis=1, concat_axis=0, tiled=True
        )
        rec_cols = lax.all_to_all(
            recurrence_output_weight, "tp", split_axis=1, concat_axis=0, tiled=True
        )
        mixed = dot(stick_all, att_cols) + dot(state_all, rec_cols)
    return mixed.astype(BF16)


def solution(mesh):
    placed = (
        P("sp", "tp"),
        P(),
        P(None, "tp"),
        P(None, "tp"),
        P(None, "tp"),
        P("tp"),
        P(None, "tp"),
        P(None, "tp"),
        P(None, "tp"),
        P(None, "tp"),
        P("tp", None),
        P("sp", "tp"),
        P(),
        P("tp", None),
        P("tp", None),
    )
    return jax.shard_map(
        shards, mesh=mesh, in_specs=placed, out_specs=P("sp", "tp"), check_vma=False
    )
```
